512 devices in a mesh: ep: 32 (over z, x), tp: 16 (over y, core).
Axes of the slice: x: 4, y: 8, z: 8, core: 2. Of those that a mesh axis runs over, the one named last changes fastest.
Arguments:
- tokens: bfloat16 [131072, 2048], P(('ep', 'tp')), may hold values from -6 to 6
- pre_gain: float32 [2048], replicated, may hold values from 0.1 to 1.9
- post_gain: float32 [2048], replicated, may hold values from 0.1 to 1.9
- expert_ids: int32 [131072, 2], P(('ep', 'tp')), may hold values from 0 to 31, as said below
- route_weight: float32 [131072, 2], P(('ep', 'tp')), may hold values from 0.1 to 1
- w_gate: bfloat16 [32, 2048, 512], P('ep', None, 'tp'), may hold values from -0.125 to 0.125
- w_up: bfloat16 [32, 2048, 512], P('ep', None, 'tp'), may hold values from -0.125 to 0.125
- w_down: bfloat16 [32, 2048, 512], P('ep', None, 'tp'), may hold values from -0.25 to 0.25
Outputs:
- layer_out: bfloat16 [131072, 2048], P(('ep', 'tp'))
The draws below stay inside these ranges and needn't reach their ends.
Inputs may be any that keep to these rules, and one draw needn't show every extreme that they name: `expert_ids`: each token names two different experts of one group, group g being experts 4 * g to 4 * g + 3. Among the rows of one device (aligned blocks of 256 rows) no expert is named more than 32 times, and in every block some expert is named exactly 32 times; one expert is named 32 times in every block.
All inputs are finite; a program needn't handle non-finite values.
Results may differ from the reference program's by a relative error of at most 0.0071.
Values may be sent and summed in bfloat16 or wider, within the bound.
A program may use at most 64 MiB of HBM per device.

```python
import math
import jax
import jax.numpy as jnp
from jax import lax

D = 2048
FF = 512
TOP = 2
GROUP = 4
TOK_DEV = 256
EXPERTS = 32
CAP = 32
TOKENS = 131072


def draw_expert_ids(key, part):
    blocks = TOKENS // TOK_DEV
    share = TOP * TOK_DEV // EXPERTS
    pairs = EXPERTS // (2 * GROUP)
    star = jax.random.randint(jax.random.fold_in(key, 11), (), 0, EXPERTS)
    star_group = star // GROUP
    star_pair = star_group // 2
    star_side = star_group % 2
    star_local = star % GROUP
    place = jnp.arange(2 * share * 2, dtype=jnp.int32)
    hot_three = 3 * share
    first_role = jnp.where(place < 2 * share, 0, jnp.where(place < hot_three, 1, jnp.where(place < hot_three + share // 2, 0, 2)))
    second_role = jnp.where(place < share, 1, jnp.where(place < 2 * share, 2, jnp.where(place < hot_three, 3, jnp.where(place < hot_three + share // 2, 1, 3))))
    is_hot = place < hot_three

    def one_block(block):
        block_key = jax.random.fold_in(key, block)
        hot_side = jax.random.randint(jax.random.fold_in(block_key, 1), (pairs,), 0, 2)
        hot_side = jnp.where(jnp.arange(pairs) == star_pair, star_side, hot_side)
        perm_keys = jax.random.split(jax.random.fold_in(block_key, 2), 2 * pairs)
        perms = jax.vmap(lambda sub: jax.random.permutation(sub, GROUP))(perm_keys).astype(jnp.int32)
        star_row = perms[star_group]
        where_star = jnp.argmax(star_row == star_local)
        star_row = star_row.at[where_star].set(star_row[0]).at[0].set(star_local)
        perms = perms.at[star_group].set(star_row)
        pair_index = jnp.arange(pairs, dtype=jnp.int32)[:, None]
        group = 2 * pair_index + jnp.where(is_hot[None, :], hot_side[:, None], 1 - hot_side[:, None])
        first = group * GROUP + perms[group, first_role[None, :]]
        second = group * GROUP + perms[group, second_role[None, :]]
        both = jnp.stack([first.reshape(-1), second.reshape(-1)], axis=1)
        shuffle = jax.random.permutation(jax.random.fold_in(block_key, 3), TOK_DEV)
        return both[shuffle]
    table = lax.map(one_block, jnp.arange(blocks, dtype=jnp.int32))
    return table.reshape(TOKENS, TOP).astype(jnp.int32)


def block_scale(rng, shape, shards, least, high):
    def one(dim, blocks):
        draws = jax.random.uniform(jax.random.fold_in(jax.random.fold_in(rng, 6), dim), (blocks,), jnp.float32, least / len(shards), high / len(shards))
        return jnp.repeat(jnp.exp(draws), shape[dim] // blocks).reshape((-1,) + (1,) * (len(shape) - dim - 1))

    level = one(*shards[0])
    for cut in shards[1:]:
        level = level * one(*cut)
    return level


def bell_draw(key, shape, spread, reach, cuts=(), kind=jnp.bfloat16):
    array = spread * jax.random.normal(key, shape, jnp.float32)
    if cuts:
        array = array * block_scale(key, shape, cuts, -0.22, 0.18)
    return jnp.clip(array, -reach, reach).astype(kind)


def setup_inputs(seed: int = 0) -> dict:
    streams_of = jax.random.split(jax.random.key(seed), 9)
    tokens = bell_draw(streams_of[0], (TOKENS, D), 1.0, 6.0, ((0, 512),))
    pre_gain = jnp.clip(1.0 + 0.18 * jax.random.normal(streams_of[1], (D,), jnp.float32), 0.1, 1.9)
    post_gain = jnp.clip(1.0 + 0.18 * jax.random.normal(streams_of[2], (D,), jnp.float32), 0.1, 1.9)
    expert_ids = draw_expert_ids(jax.random.fold_in(streams_of[8], 71), 0)
    route_weight = jnp.clip(jnp.exp(math.log(1.0) - 2.3025851 * jax.random.uniform(streams_of[4], (TOKENS, TOP), jnp.float32) ** block_scale(streams_of[4], (TOKENS, TOP), ((0, 512),), -0.2, 0.2)), 0.1, 1.0)
    w_gate = bell_draw(streams_of[5], (EXPERTS, D, FF), D ** -0.5, 0.125, ((0, 32), (2, 16)))
    w_up = bell_draw(streams_of[6], (EXPERTS, D, FF), D ** -0.5, 0.125, ((0, 32), (2, 16)))
    w_down = bell_draw(streams_of[7], (EXPERTS, D, FF), FF ** -0.5, 0.25, ((0, 32), (2, 16)))
    return dict(tokens=tokens, pre_gain=pre_gain, post_gain=post_gain, expert_ids=expert_ids, route_weight=route_weight, w_gate=w_gate, w_up=w_up, w_down=w_down)


def rms_scale(values, gain):
    mean_sq = lax.optimization_barrier(jnp.mean(values * values, axis=-1, keepdims=True))
    return values * lax.rsqrt(mean_sq + 1e-06) * gain

def reference(tokens, pre_gain, post_gain, expert_ids, route_weight, w_gate, w_up, w_down):
    count = tokens.shape[0]
    width = tokens.shape[1]
    normed = rms_scale(tokens.astype(jnp.float32), pre_gain).astype(jnp.bfloat16)
    padded = jnp.concatenate([normed, jnp.zeros((1, width), jnp.bfloat16)], axis=0)
    flat = expert_ids.reshape(-1).astype(jnp.int32)
    routes = flat.shape[0]
    order = jnp.argsort(flat, stable=True).astype(jnp.int32)
    sorted_ids = flat[order]
    first = jnp.searchsorted(sorted_ids, sorted_ids, side='left').astype(jnp.int32)
    rank = jnp.arange(routes, dtype=jnp.int32) - first
    global_cap = count // TOK_DEV * CAP
    table = jnp.full((EXPERTS * global_cap,), routes, jnp.int32)
    table = table.at[sorted_ids * global_cap + rank].set(order).reshape(EXPERTS, global_cap)

    def one_expert(index):
        slots = table[index]
        rows = padded[jnp.minimum(slots // TOP, count).astype(jnp.int32)]
        rows = jnp.where((slots < routes)[:, None], rows, jnp.zeros_like(rows))
        gate = jnp.dot(rows, w_gate[index], preferred_element_type=jnp.float32)
        up = jnp.dot(rows, w_up[index], preferred_element_type=jnp.float32)
        hidden = (jax.nn.silu(gate) * up).astype(jnp.bfloat16)
        return jnp.dot(hidden, w_down[index].T, preferred_element_type=jnp.float32).astype(jnp.bfloat16)
    results = lax.map(one_expert, jnp.arange(EXPERTS, dtype=jnp.int32))
    per_route = jnp.zeros((routes + 1, width), jnp.bfloat16)
    per_route = per_route.at[table.reshape(-1)].set(results.reshape(-1, width))
    per_route = per_route[:routes].reshape(count, TOP, width)
    mixed = lax.optimization_barrier(jnp.sum(per_route.astype(jnp.float32) * route_weight[:, :, None], axis=1))
    return rms_scale(mixed, post_gain).astype(jnp.bfloat16)
```

```python
import jax
import jax.numpy as jnp
from jax import lax
from jax.experimental import pallas as pl
from jax.experimental.pallas import tpu as pltpu
from jax.sharding import PartitionSpec as P

MESH = pl.DeviceIdType.MESH
BF16 = jnp.bfloat16
F32 = jnp.float32
WIDTH = 2048
TOKENS = 256
PART = 32
FF = 512
ZS = 8
XS = 4
YS = 8
SLOT = 64
CAP = 32
COLS = 512
DELTA = (2, 6, 1, 7, 3, 5, 4, 0)
OWN = 7
STEP_X = (1, 3, 2)


def nt_dot(a, b):
    return lax.dot_general(a, b, (((1,), (1,)), ((), ())), preferred_element_type=F32)


def tn_dot(a, b):
    return lax.dot_general(a, b, (((0,), (0,)), ((), ())), preferred_element_type=F32)


def nn_dot(a, b):
    return jnp.dot(a, b, preferred_element_type=F32)


def iota(shape, dim):
    return lax.broadcasted_iota(jnp.int32, shape, dim)


def rms_scale(values, gain):
    mean_sq = jnp.mean(values * values, axis=-1, keepdims=True)
    return values * lax.rsqrt(mean_sq + 1e-06) * gain


def kernel(
    tok_ref, pre_ref, post_ref, ids_ref, rw_ref, wg_ref, wu_ref, wd_ref, out_ref,
    normed, onehot, zsend, msend, zrecv, mrecv, xsend, xrecv, wall, ores, xret, zback, zfin, mixed,
    zs_sem, zr_sem, ms_sem, mr_sem, xs_sem, xr_sem, os_sem, or_sem, bs_sem, br_sem,
    ws_sem, wr_sem, ds_sem, dr_sem,
):
    ep, tp = lax.axis_index("ep"), lax.axis_index("tp")
    z, x = ep // XS, ep % XS
    y, core = tp // 2, tp % 2

    def at_z(step):
        return (lax.rem(z + step, ZS) * XS + x, tp)

    def at_x(step):
        return (z * XS + lax.rem(x + step, XS), tp)

    def at_y(step):
        return (ep, lax.rem(y + step, YS) * 2 + core)

    other = (ep, y * 2 + (1 - core))

    def remote(src, dst, send, recv, device):
        return pltpu.make_async_remote_copy(
            src_ref=src, dst_ref=dst, send_sem=send, recv_sem=recv,
            device_id=device, device_id_type=MESH,
        )

    barrier = pltpu.get_barrier_semaphore()
    partners = [at_z(k) for k in range(1, ZS)] + [at_x(k) for k in range(1, XS)]
    partners += [at_y(1), at_y(YS - 1), other]
    for device in partners:
        pl.semaphore_signal(barrier, inc=1, device_id=device, device_id_type=MESH)

    for m, ref in enumerate((wg_ref, wu_ref, wd_ref)):
        wall[m, 0] = ref[...]
    for r in range(0, TOKENS, 32):
        rows = tok_ref[pl.ds(r, 32), :].astype(F32)
        normed[pl.ds(r, 32), :] = rms_scale(rows, pre_ref[...]).astype(BF16)
    ids0, ids1 = ids_ref[0:1, :], ids_ref[1:2, :]
    rw0, rw1 = rw_ref[0:1, :], rw_ref[1:2, :]
    before = (iota((TOKENS, TOKENS), 0) < iota((TOKENS, TOKENS), 1)).astype(F32).astype(BF16)
    row = iota((ZS * 8, 1), 0)
    place = row // 8
    delta = jnp.zeros_like(place)
    for p, d in enumerate(DELTA):
        delta = jnp.where(place == p, d, delta)
    home = lax.rem(z + delta, ZS)
    expert = jnp.where(row % 8 < XS, home * XS + row % 8, -1)
    first, second = ids0 == expert, ids1 == expert
    chosen = (first | second).astype(F32)
    rank = nn_dot(chosen.astype(BF16), before)
    rank1 = (rank + 1.0) * chosen
    weight = jnp.where(first, rw0, 0.0) + jnp.where(second, rw1, 0.0)
    w_hi = weight.astype(BF16).astype(F32)
    w_lo = weight - w_hi
    place8 = iota((ZS, 1), 0)
    delta8 = jnp.zeros_like(place8)
    for p, d in enumerate(DELTA):
        delta8 = jnp.where(place8 == p, d, delta8)
    in_group = (ids0 // XS == lax.rem(z + delta8, ZS)).astype(F32)
    slot_all = nn_dot(in_group.astype(BF16), before)
    spot = jnp.sum(
        in_group * (slot_all + (place8 * SLOT).astype(F32)), axis=0, keepdims=True
    ).astype(jnp.int32)
    for p in range(ZS):
        onehot[p] = (iota((SLOT, TOKENS), 0) + p * SLOT == spot).astype(F32).astype(BF16)

    pl.semaphore_wait(barrier, len(partners))

    def ring(step):
        if step < 4:
            ahead = (wall.at[:, step - 1], wall.at[:, step])
            back = (wall.at[:, (YS - step + 1) % YS], wall.at[:, YS - step])
        else:
            low, high = pl.ds(0, PART // 2), pl.ds(PART // 2, PART // 2)
            ahead = (wall.at[:, 3, low], wall.at[:, 4, low])
            back = (wall.at[:, 5, high], wall.at[:, 4, high])
        k = step - 1
        return [
            remote(*ahead, ws_sem.at[0, k], wr_sem.at[0, k], at_y(1)),
            remote(*back, ws_sem.at[1, k], wr_sem.at[1, k], at_y(YS - 1)),
        ]

    rings = {step: ring(step) for step in (1, 2, 3, 4)}
    dies = [
        remote(wall.at[:, m], wall.at[:, YS + m], ds_sem.at[m], dr_sem.at[m], other)
        for m in range(YS)
    ]

    def relay(step):
        for copy in rings[step]:
            copy.wait_recv()
        if step < 4:
            for copy in rings[step + 1]:
                copy.start()
        for m in (step, YS - step) if step < 4 else (4,):
            dies[m].start()

    for copy in rings[1]:
        copy.start()
    dies[0].start()

    z_out, m_out = {}, {}

    def send_plane(p):
        chosen_rows = onehot[p]
        meta = jnp.concatenate(
            [rank1[8 * p : 8 * p + 8], w_hi[8 * p : 8 * p + 8], w_lo[8 * p : 8 * p + 8],
             jnp.zeros((8, TOKENS), F32)], axis=0,
        ).astype(BF16)
        meta = nt_dot(meta, chosen_rows).astype(BF16)
        meta = jnp.concatenate([meta, jnp.zeros((32, 128 - SLOT), BF16)], axis=1)
        to_rows, to_meta = (zrecv, mrecv) if p == OWN else (zsend, msend)
        to_meta[p] = meta
        for c in range(0, WIDTH, COLS):
            part = nn_dot(chosen_rows, normed[:, c : c + COLS])
            to_rows[p, :, c : c + COLS] = part.astype(BF16)
        if p != OWN:
            m_out[p] = remote(msend.at[p], mrecv.at[p], ms_sem.at[p], mr_sem.at[p], at_z(DELTA[p]))
            z_out[p] = remote(zsend.at[p], zrecv.at[p], zs_sem.at[p], zr_sem.at[p], at_z(DELTA[p]))
            m_out[p].start()
            z_out[p].start()

    def selector(p):
        meta = mrecv[p].astype(F32)[:, :SLOT]
        want = (iota((CAP, SLOT), 0) + 1).astype(F32)
        return meta, [(meta[i : i + 1, :] == want).astype(F32) for i in range(XS)]

    x_out, o_out = {}, {}

    def send_experts(p):
        if p != OWN:
            m_out[p].wait_recv()
            z_out[p].wait_recv()
        pick = jnp.concatenate(selector(p)[1], axis=0).astype(BF16)
        for c in range(0, WIDTH, COLS):
            part = nn_dot(pick, zrecv[p, :, c : c + COLS]).astype(BF16)
            xsend[p, :, :, c : c + COLS] = part.reshape(XS, CAP, COLS)
        for j, step in enumerate(STEP_X):
            x_out[p, j] = remote(
                xsend.at[p, lax.rem(x + step, XS)], xrecv.at[p, j + 1],
                xs_sem.at[p, j], xr_sem.at[p, j], at_x(step),
            )
            x_out[p, j].start()
        xrecv[p, 0] = xsend[p, x]

    def experts(p):
        for q in (p, p + 1):
            for j in range(XS - 1):
                x_out[q, j].wait_recv()
        rows = xrecv[pl.ds(p, 2)].reshape(2 * XS * CAP, WIDTH)
        gate = nt_dot(rows, wall[0].reshape(FF, WIDTH))
        up = nt_dot(rows, wall[1].reshape(FF, WIDTH))
        hidden = (gate / (1.0 + jnp.exp(-gate)) * up).astype(BF16)
        for c in range(0, WIDTH, COLS):
            part = nn_dot(hidden, wall[2, :, :, c : c + COLS].reshape(FF, COLS)).astype(BF16)
            ores[pl.ds(p, 2), :, :, c : c + COLS] = part.reshape(2, XS, CAP, COLS)
        for q in (p, p + 1):
            for j, step in enumerate(STEP_X):
                o_out[q, j] = remote(
                    ores.at[q, j + 1], xret.at[q, x],
                    os_sem.at[q, j], or_sem.at[q, j], at_x(XS - step),
                )
                o_out[q, j].start()
            xret[q, x] = ores[q, 0]

    b_out = {}

    def combine(p):
        for j, step in enumerate(STEP_X):
            remote(
                ores.at[p, j + 1], xret.at[p, lax.rem(x + step, XS)],
                os_sem.at[p, j], or_sem.at[p, j], at_x(XS - step),
            ).wait_recv()
        meta, picks = selector(p)
        hi = jnp.concatenate(
            [pick * meta[8 + i : 9 + i, :] for i, pick in enumerate(picks)], axis=0
        ).astype(BF16)
        lo = jnp.concatenate(
            [pick * meta[16 + i : 17 + i, :] for i, pick in enumerate(picks)], axis=0
        ).astype(BF16)
        to_rows = zfin if p == OWN else zback
        for c in range(0, WIDTH, COLS):
            rows = xret[p, :, :, c : c + COLS].reshape(XS * CAP, COLS)
            to_rows[p, :, c : c + COLS] = (tn_dot(hi, rows) + tn_dot(lo, rows)).astype(BF16)
        if p != OWN:
            b_out[p] = remote(
                zback.at[p], zfin.at[p], bs_sem.at[p], br_sem.at[p], at_z(ZS - DELTA[p])
            )
            b_out[p].start()

    send_plane(2)
    send_plane(3)
    send_plane(OWN)
    send_experts(OWN)
    for p in (0, 1, 4, 5, 6):
        send_plane(p)
    send_experts(2)
    send_experts(3)
    relay(1)
    send_experts(0)
    send_experts(1)
    relay(2)
    relay(3)
    send_experts(4)
    send_experts(5)
    relay(4)
    for copy in dies:
        copy.wait_recv()
    experts(0)
    send_experts(6)
    experts(2)
    combine(0)
    combine(1)
    experts(4)
    combine(2)
    combine(3)
    experts(6)
    combine(4)
    combine(5)
    combine(6)
    combine(7)
    for p in range(ZS - 1):
        b_out[p].wait_recv()
    for c in range(0, WIDTH, COLS):
        rows = zfin[:, :, c : c + COLS].reshape(ZS * SLOT, COLS)
        mixed[:, c : c + COLS] = tn_dot(onehot[...].reshape(ZS * SLOT, TOKENS), rows)
    for r in range(0, TOKENS, 32):
        out_ref[pl.ds(r, 32), :] = rms_scale(mixed[pl.ds(r, 32), :], post_ref[...]).astype(BF16)
    for step in rings:
        for copy in rings[step]:
            copy.wait_send()
    for copies in (dies, m_out.values(), z_out.values(), x_out.values(), o_out.values(), b_out.values()):
        for copy in copies:
            copy.wait_send()


def body(tokens, pre_gain, post_gain, expert_ids, route_weight, w_gate, w_up, w_down):
    dma = pltpu.SemaphoreType.DMA
    vmem = pltpu.VMEM
    return pl.pallas_call(
        kernel,
        name="experts",
        out_shape=jax.ShapeDtypeStruct((TOKENS, WIDTH), BF16),
        in_specs=[pl.BlockSpec(memory_space=vmem)] * 8,
        out_specs=pl.BlockSpec(memory_space=vmem),
        scratch_shapes=[
            vmem((TOKENS, WIDTH), BF16),
            vmem((ZS, SLOT, TOKENS), BF16),
            vmem((ZS, SLOT, WIDTH), BF16),
            vmem((ZS, 32, 128), BF16),
            vmem((ZS, SLOT, WIDTH), BF16),
            vmem((ZS, 32, 128), BF16),
            vmem((ZS, XS, CAP, WIDTH), BF16),
            vmem((ZS, XS, CAP, WIDTH), BF16),
            vmem((3, 2 * YS, PART, WIDTH), BF16),
            vmem((ZS, XS, CAP, WIDTH), BF16),
            vmem((ZS, XS, CAP, WIDTH), BF16),
            vmem((ZS, SLOT, WIDTH), BF16),
            vmem((ZS, SLOT, WIDTH), BF16),
            vmem((TOKENS, WIDTH), F32),
            dma((ZS,)), dma((ZS,)), dma((ZS,)), dma((ZS,)),
            dma((ZS, XS - 1)), dma((ZS, XS - 1)), dma((ZS, XS - 1)), dma((ZS, XS - 1)),
            dma((ZS,)), dma((ZS,)),
            dma((2, 4)), dma((2, 4)), dma((YS,)), dma((YS,)),
        ],
        compiler_params=pltpu.CompilerParams(
            collective_id=0, has_side_effects=True, vmem_limit_bytes=60 << 20
        ),
    )(
        tokens, pre_gain[None], post_gain[None], expert_ids.T, route_weight.T,
        w_gate[0].T, w_up[0].T, w_down[0].T,
    )


def solution(mesh):
    in_specs = (
        P(("ep", "tp"), None),
        P(),
        P(),
        P(("ep", "tp"), None),
        P(("ep", "tp"), None),
        P("ep", None, "tp"),
        P("ep", None, "tp"),
        P("ep", None, "tp"),
    )
    out_specs = P(("ep", "tp"), None)
    return jax.shard_map(body, mesh=mesh, in_specs=in_specs, out_specs=out_specs, check_vma=False)
```

```python
import jax
import jax.numpy as jnp
from jax import lax
from jax.experimental import pallas as pl
from jax.experimental.pallas import tpu as pltpu
from jax.sharding import PartitionSpec as P

MESH = pl.DeviceIdType.MESH
BF16 = jnp.bfloat16
F32 = jnp.float32
WIDTH = 2048
TOKENS = 256
PART = 32
FF = 512
ZS = 8
XS = 4
YS = 8
SLOT = 64
CAP = 32
COLS = 512
DELTA = (1, 7, 2, 6, 3, 5, 0, 4)
STEP = (1, 7, 2, 6, 7, 1, 0, 0)
LOCAL = (6, 7)
STEP_X = (1, 3, 2)
HALF = PART // 2


def nt_dot(a, b):
    return lax.dot_general(a, b, (((1,), (1,)), ((), ())), preferred_element_type=F32)


def tn_dot(a, b):
    return lax.dot_general(a, b, (((0,), (0,)), ((), ())), preferred_element_type=F32)


def nn_dot(a, b):
    return jnp.dot(a, b, preferred_element_type=F32)


def iota(shape, dim):
    return lax.broadcasted_iota(jnp.int32, shape, dim)


def rms_scale(values, gain):
    mean_sq = jnp.mean(values * values, axis=-1, keepdims=True)
    return values * lax.rsqrt(mean_sq + 1e-06) * gain


def kernel(
    tok_hbm, pre_hbm, post_hbm, ids_hbm, rw_hbm, wg_hbm, wu_hbm, wd_hbm, out_ref,
    tok_ref, pre_ref, post_ref, ids_ref, rw_ref, in_sem, normed, onehot, zsend, msend, zrecv, mrecv, xsend, xrecv, near, far, ores, xret, zback, zfin, mixed,
    zs_sem, zr_sem, ms_sem, mr_sem, xs_sem, xr_sem, os_sem, or_sem, bs_sem, br_sem,
    ws_sem, wr_sem, ds_sem, dr_sem, fs_sem, fr_sem, gs_sem, gr_sem, hs_sem, hr_sem,
):
    ep, tp = lax.axis_index("ep"), lax.axis_index("tp")
    z, x = ep // XS, ep % XS
    y, core = tp // 2, tp % 2

    def at_z(step):
        return (lax.rem(z + step, ZS) * XS + x, tp)

    def at_x(step):
        return (z * XS + lax.rem(x + step, XS), tp)

    def at_y(step):
        return (ep, lax.rem(y + step, YS) * 2 + core)

    other = (ep, y * 2 + (1 - core))

    def remote(src, dst, send, recv, device):
        return pltpu.make_async_remote_copy(
            src_ref=src, dst_ref=dst, send_sem=send, recv_sem=recv,
            device_id=device, device_id_type=MESH,
        )

    loads = [
        pltpu.make_async_copy(src, dst, in_sem.at[k])
        for k, (src, dst) in enumerate((
            (tok_hbm, tok_ref), (pre_hbm, pre_ref), (ids_hbm, ids_ref), (rw_hbm, rw_ref),
            (wg_hbm, near.at[0, 0]), (wu_hbm, near.at[1, 0]), (wd_hbm, near.at[2, 0]),
            (post_hbm, post_ref),
        ))
    ]
    for copy in loads:
        copy.start()
    barrier = pltpu.get_barrier_semaphore()
    partners = [at_z(k) for k in (1, 2, 4, 6, 7)] + [at_x(k) for k in range(1, XS)]
    partners += [at_y(1), at_y(YS - 1), other]
    for device in partners:
        pl.semaphore_signal(barrier, inc=1, device_id=device, device_id_type=MESH)

    for copy in loads:
        copy.wait()
    for r in range(0, TOKENS, 32):
        rows = tok_ref[pl.ds(r, 32), :].astype(F32)
        normed[pl.ds(r, 32), :] = rms_scale(rows, pre_ref[...]).astype(BF16)
    ids0, ids1 = ids_ref[0:1, :], ids_ref[1:2, :]
    rw0, rw1 = rw_ref[0:1, :], rw_ref[1:2, :]
    before = (iota((TOKENS, TOKENS), 0) < iota((TOKENS, TOKENS), 1)).astype(F32).astype(BF16)

    def home_of(place):
        delta = jnp.zeros_like(place)
        for p, d in enumerate(DELTA):
            delta = jnp.where(place == p, d, delta)
        return lax.rem(z + delta, ZS)

    row = iota((ZS * 8, 1), 0)
    expert = jnp.where(row % 8 < XS, home_of(row // 8) * XS + row % 8, -1)
    first, second = ids0 == expert, ids1 == expert
    chosen = (first | second).astype(F32)
    rank1 = (nn_dot(chosen.astype(BF16), before) + 1.0) * chosen
    weight = jnp.where(first, rw0, 0.0) + jnp.where(second, rw1, 0.0)
    w_hi = weight.astype(BF16).astype(F32)
    w_lo = weight - w_hi
    place8 = iota((ZS, 1), 0)
    in_group = (ids0 // XS == home_of(place8)).astype(F32)
    slot = nn_dot(in_group.astype(BF16), before) + (place8 * SLOT).astype(F32)
    spot = jnp.sum(in_group * slot, axis=0, keepdims=True).astype(jnp.int32)
    for p in range(ZS):
        onehot[p] = (iota((SLOT, TOKENS), 0) + p * SLOT == spot).astype(F32).astype(BF16)

    pl.semaphore_wait(barrier, len(partners))

    def part(name, m, h):
        return near.at[:, m, pl.ds(h * HALF, HALF)] if name == "near" else far.at[h, m]

    def ring(name, h, step, send, recv):
        k = step - 1
        pairs = [
            (part(name, step - 1, h), part(name, step, h)),
            (part(name, (YS - step + 1) % YS, h), part(name, YS - step, h)),
        ]
        if step == 4 and name == "near":
            pairs[1 - h] = None
        elif step == 4:
            low, high = pl.ds(0, HALF), pl.ds(HALF, HALF)
            pairs = [
                (far.at[h, 3, low], far.at[h, 4, low]),
                (far.at[h, 5, high], far.at[h, 4, high]),
            ]
        return [
            remote(*pair, send.at[h, way, k], recv.at[h, way, k], at_y((1, YS - 1)[way]))
            for way, pair in enumerate(pairs) if pair is not None
        ]

    rings, dies = {}, {}
    for name, count, sems in (
        ("near", 2, (ws_sem, wr_sem, ds_sem, dr_sem)), ("far", 3, (fs_sem, fr_sem, gs_sem, gr_sem))
    ):
        for h in range(count):
            for step in (1, 2, 3, 4):
                rings[name, h, step] = ring(name, h, step, *sems[:2])
            for m in range(YS):
                dies[name, h, m] = remote(
                    part(name, m, h), part(name, YS + m, h), sems[2].at[h, m], sems[3].at[h, m], other
                )

    shards = [
        remote(near.at[h, 0], far.at[h, 0], hs_sem.at[h], hr_sem.at[h], at_z(4)) for h in range(3)
    ]

    def relay(name, h, step):
        if step == 0:
            if name == "far":
                shards[h].wait_recv()
        else:
            for copy in rings[name, h, step]:
                copy.wait_recv()
        if step < 4:
            for copy in rings[name, h, step + 1]:
                copy.start()
        for m in sorted({step, (YS - step) % YS}):
            dies[name, h, m].start()

    def whole(name):
        for key, copy in dies.items():
            if key[0] == name:
                copy.wait_recv()

    z_out, m_out = {}, {}

    def send_plane(p):
        chosen_rows = onehot[p]
        meta = jnp.concatenate(
            [rank1[8 * p : 8 * p + 8], w_hi[8 * p : 8 * p + 8], w_lo[8 * p : 8 * p + 8],
             jnp.zeros((8, TOKENS), F32)], axis=0,
        ).astype(BF16)
        meta = nt_dot(meta, chosen_rows).astype(BF16)
        meta = jnp.concatenate([meta, jnp.zeros((32, 128 - SLOT), BF16)], axis=1)
        to_rows, to_meta = (zrecv, mrecv) if p in LOCAL else (zsend, msend)
        to_meta[p] = meta
        for c in range(0, WIDTH, COLS):
            block = nn_dot(chosen_rows, normed[:, c : c + COLS])
            to_rows[p, :, c : c + COLS] = block.astype(BF16)
        if p not in LOCAL:
            m_out[p] = remote(msend.at[p], mrecv.at[p], ms_sem.at[p], mr_sem.at[p], at_z(STEP[p]))
            z_out[p] = remote(zsend.at[p], zrecv.at[p], zs_sem.at[p], zr_sem.at[p], at_z(STEP[p]))
            m_out[p].start()
            z_out[p].start()

    def selector(p):
        meta = mrecv[p].astype(F32)[:, :SLOT]
        want = (iota((CAP, SLOT), 0) + 1).astype(F32)
        return meta, [(meta[i : i + 1, :] == want).astype(F32) for i in range(XS)]

    x_out, o_out = {}, {}

    def send_experts(p):
        if p not in LOCAL:
            m_out[p].wait_recv()
            z_out[p].wait_recv()
        pick = jnp.concatenate(selector(p)[1], axis=0).astype(BF16)
        for c in range(0, WIDTH, COLS):
            block = nn_dot(pick, zrecv[p, :, c : c + COLS]).astype(BF16)
            xsend[p, :, :, c : c + COLS] = block.reshape(XS, CAP, COLS)
        for j, step in enumerate(STEP_X):
            x_out[p, j] = remote(
                xsend.at[p, lax.rem(x + step, XS)], xrecv.at[p, j + 1],
                xs_sem.at[p, j], xr_sem.at[p, j], at_x(step),
            )
            x_out[p, j].start()
        xrecv[p, 0] = xsend[p, x]

    def experts(p, count, weights):
        for q in range(p, p + count):
            for j in range(XS - 1):
                x_out[q, j].wait_recv()
        rows = xrecv[pl.ds(p, count)].reshape(count * XS * CAP, WIDTH)
        gate = nt_dot(rows, weights[0].reshape(FF, WIDTH))
        up = nt_dot(rows, weights[1].reshape(FF, WIDTH))
        hidden = (gate / (1.0 + jnp.exp(-gate)) * up).astype(BF16)
        for c in range(0, WIDTH, COLS):
            block = nn_dot(hidden, weights[2, :, :, c : c + COLS].reshape(FF, COLS)).astype(BF16)
            ores[pl.ds(p, count), :, :, c : c + COLS] = block.reshape(count, XS, CAP, COLS)
        for q in range(p, p + count):
            for j, step in enumerate(STEP_X):
                o_out[q, j] = remote(
                    ores.at[q, j + 1], xret.at[q, x],
                    os_sem.at[q, j], or_sem.at[q, j], at_x(XS - step),
                )
                o_out[q, j].start()
            xret[q, x] = ores[q, 0]

    b_out = {}

    def combine(p):
        for j, step in enumerate(STEP_X):
            remote(
                ores.at[p, j + 1], xret.at[p, lax.rem(x + step, XS)],
                os_sem.at[p, j], or_sem.at[p, j], at_x(XS - step),
            ).wait_recv()
        meta, picks = selector(p)
        hi = jnp.concatenate(
            [pick * meta[8 + i : 9 + i, :] for i, pick in enumerate(picks)], axis=0
        ).astype(BF16)
        lo = jnp.concatenate(
            [pick * meta[16 + i : 17 + i, :] for i, pick in enumerate(picks)], axis=0
        ).astype(BF16)
        to_rows = zfin if p in LOCAL else zback
        for c in range(0, WIDTH, COLS):
            rows = xret[p, :, :, c : c + COLS].reshape(XS * CAP, COLS)
            to_rows[p, :, c : c + COLS] = (tn_dot(hi, rows) + tn_dot(lo, rows)).astype(BF16)
        if p not in LOCAL:
            b_out[p] = remote(
                zback.at[p], zfin.at[p], bs_sem.at[p], br_sem.at[p], at_z(ZS - STEP[p])
            )
            b_out[p].start()

    relay("near", 0, 0)
    relay("near", 1, 0)
    send_plane(6)
    send_experts(6)
    send_plane(0)
    send_plane(1)
    send_plane(7)
    send_experts(7)
    send_plane(4)
    send_plane(5)
    shards[0].start()
    send_plane(2)
    send_plane(3)
    relay("near", 0, 1)
    send_experts(0)
    send_experts(1)
    relay("near", 1, 1)
    relay("near", 0, 2)
    relay("near", 1, 2)
    send_experts(4)
    send_experts(5)
    relay("near", 0, 3)
    relay("near", 1, 3)
    relay("far", 0, 0)
    relay("near", 0, 4)
    relay("near", 1, 4)
    send_experts(2)
    send_experts(3)
    shards[1].start()
    shards[2].start()
    relay("far", 0, 1)
    relay("far", 0, 2)
    whole("near")
    experts(0, 2, near)
    relay("far", 1, 0)
    relay("far", 0, 3)
    relay("far", 1, 1)
    relay("far", 2, 0)
    experts(2, 2, near)
    relay("far", 0, 4)
    relay("far", 1, 2)
    relay("far", 2, 1)
    experts(6, 1, near)
    relay("far", 1, 3)
    relay("far", 2, 2)
    combine(0)
    combine(1)
    relay("far", 1, 4)
    relay("far", 2, 3)
    combine(2)
    relay("far", 2, 4)
    whole("far")
    experts(4, 2, far)
    combine(3)
    experts(7, 1, far)
    combine(6)
    combine(4)
    combine(5)
    combine(7)
    for p in range(ZS):
        if p not in LOCAL:
            b_out[p].wait_recv()
    for c in range(0, WIDTH, COLS):
        rows = zfin[:, :, c : c + COLS].reshape(ZS * SLOT, COLS)
        mixed[:, c : c + COLS] = tn_dot(onehot[...].reshape(ZS * SLOT, TOKENS), rows)
    for r in range(0, TOKENS, 32):
        out_ref[pl.ds(r, 32), :] = rms_scale(mixed[pl.ds(r, 32), :], post_ref[...]).astype(BF16)
    for copies in [*rings.values(), dies.values(), shards]:
        for copy in copies:
            copy.wait_send()
    for copies in (m_out, z_out, x_out, o_out, b_out):
        for copy in copies.values():
            copy.wait_send()


def body(tokens, pre_gain, post_gain, expert_ids, route_weight, w_gate, w_up, w_down):
    dma = pltpu.SemaphoreType.DMA
    vmem = pltpu.VMEM
    return pl.pallas_call(
        kernel,
        name="experts",
        out_shape=jax.ShapeDtypeStruct((TOKENS, WIDTH), BF16),
        in_specs=[pl.BlockSpec(memory_space=pltpu.HBM)] * 8,
        out_specs=pl.BlockSpec(memory_space=vmem),
        scratch_shapes=[
            vmem((TOKENS, WIDTH), BF16),
            vmem((1, WIDTH), F32),
            vmem((1, WIDTH), F32),
            vmem((2, TOKENS), jnp.int32),
            vmem((2, TOKENS), F32),
            dma((8,)),
            vmem((TOKENS, WIDTH), BF16),
            vmem((ZS, SLOT, TOKENS), BF16),
            vmem((ZS, SLOT, WIDTH), BF16),
            vmem((ZS, 32, 128), BF16),
            vmem((ZS, SLOT, WIDTH), BF16),
            vmem((ZS, 32, 128), BF16),
            vmem((ZS, XS, CAP, WIDTH), BF16),
            vmem((ZS, XS, CAP, WIDTH), BF16),
            vmem((3, 2 * YS, PART, WIDTH), BF16),
            vmem((3, 2 * YS, PART, WIDTH), BF16),
            vmem((ZS, XS, CAP, WIDTH), BF16),
            vmem((ZS, XS, CAP, WIDTH), BF16),
            vmem((ZS, SLOT, WIDTH), BF16),
            vmem((ZS, SLOT, WIDTH), BF16),
            vmem((TOKENS, WIDTH), F32),
            dma((ZS,)), dma((ZS,)), dma((ZS,)), dma((ZS,)),
            dma((ZS, XS - 1)), dma((ZS, XS - 1)), dma((ZS, XS - 1)), dma((ZS, XS - 1)),
            dma((ZS,)), dma((ZS,)),
            dma((2, 2, 4)), dma((2, 2, 4)), dma((2, YS)), dma((2, YS)),
            dma((3, 2, 4)), dma((3, 2, 4)), dma((3, YS)), dma((3, YS)), dma((3,)), dma((3,)),
        ],
        compiler_params=pltpu.CompilerParams(
            collective_id=0, has_side_effects=True, vmem_limit_bytes=52 << 20
        ),
    )(*[
        pltpu.with_memory_space_constraint(a, pltpu.HBM)
        for a in (
            tokens, pre_gain[None], post_gain[None], expert_ids.T, route_weight.T,
            w_gate[0].T, w_up[0].T, w_down[0].T,
        )
    ])


def solution(mesh):
    in_specs = (
        P(("ep", "tp"), None),
        P(),
        P(),
        P(("ep", "tp"), None),
        P(("ep", "tp"), None),
        P("ep", None, "tp"),
        P("ep", None, "tp"),
        P("ep", None, "tp"),
    )
    out_specs = P(("ep", "tp"), None)
    return jax.shard_map(body, mesh=mesh, in_specs=in_specs, out_specs=out_specs, check_vma=False)
```

```python
import jax
import jax.numpy as jnp
from jax import lax
from jax.experimental import pallas as pl
from jax.experimental.pallas import tpu as pltpu
from jax.sharding import PartitionSpec as P

MESH = pl.DeviceIdType.MESH
BF16 = jnp.bfloat16
F32 = jnp.float32
WIDTH = 2048
TOKENS = 256
PART = 32
FF = 512
ZS = 8
XS = 4
YS = 8
SLOT = 64
CAP = 32
COLS = 512
DELTA = (1, 7, 2, 6, 3, 5, 0, 4)
STEP = (1, 7, 2, 6, 7, 1, 0, 0)
LOCAL = (6, 7)
STEP_X = (1, 3, 2)
HALF = PART // 2


def nt_dot(a, b):
    return lax.dot_general(a, b, (((1,), (1,)), ((), ())), preferred_element_type=F32)


def tn_dot(a, b):
    return lax.dot_general(a, b, (((0,), (0,)), ((), ())), preferred_element_type=F32)


def nn_dot(a, b):
    return jnp.dot(a, b, preferred_element_type=F32)


def iota(shape, dim):
    return lax.broadcasted_iota(jnp.int32, shape, dim)


def rms_scale(values, gain):
    mean_sq = jnp.mean(values * values, axis=-1, keepdims=True)
    return values * lax.rsqrt(mean_sq + 1e-06) * gain


def kernel(
    tok_hbm, pre_hbm, post_hbm, ids_hbm, rw_hbm, wg_hbm, wu_hbm, wd_hbm, out_ref,
    tok_ref, pre_ref, post_ref, ids_ref, rw_ref, in_sem, normed, onehot, zsend, msend, zrecv, mrecv, xsend, xrecv, near, far, ores, xret, zback, zfin, mixed,
    zs_sem, zr_sem, ms_sem, mr_sem, xs_sem, xr_sem, os_sem, or_sem, bs_sem, br_sem,
    ws_sem, wr_sem, ds_sem, dr_sem, fs_sem, fr_sem, gs_sem, gr_sem, hs_sem, hr_sem,
):
    ep, tp = lax.axis_index("ep"), lax.axis_index("tp")
    z, x = ep // XS, ep % XS
    y, core = tp // 2, tp % 2

    def at_z(step):
        return (lax.rem(z + step, ZS) * XS + x, tp)

    def at_x(step):
        return (z * XS + lax.rem(x + step, XS), tp)

    def at_y(step):
        return (ep, lax.rem(y + step, YS) * 2 + core)

    other = (ep, y * 2 + (1 - core))

    def remote(src, dst, send, recv, device):
        return pltpu.make_async_remote_copy(
            src_ref=src, dst_ref=dst, send_sem=send, recv_sem=recv,
            device_id=device, device_id_type=MESH,
        )

    loads = [
        pltpu.make_async_copy(src, dst, in_sem.at[k])
        for k, (src, dst) in enumerate((
            (tok_hbm, tok_ref), (pre_hbm, pre_ref), (ids_hbm, ids_ref), (rw_hbm, rw_ref),
            (wg_hbm, near.at[0, 0]), (wu_hbm, near.at[1, 0]), (wd_hbm, near.at[2, 0]),
            (post_hbm, post_ref),
        ))
    ]
    for copy in loads:
        copy.start()
    barrier = pltpu.get_barrier_semaphore()
    partners = [at_z(k) for k in (1, 2, 4, 6, 7)] + [at_x(k) for k in range(1, XS)]
    partners += [at_y(1), at_y(YS - 1), other]
    for device in partners:
        pl.semaphore_signal(barrier, inc=1, device_id=device, device_id_type=MESH)

    for copy in loads:
        copy.wait()
    for r in range(0, TOKENS, 32):
        rows = tok_ref[pl.ds(r, 32), :].astype(F32)
        normed[pl.ds(r, 32), :] = rms_scale(rows, pre_ref[...]).astype(BF16)
    ids0, ids1 = ids_ref[0:1, :], ids_ref[1:2, :]
    rw0, rw1 = rw_ref[0:1, :], rw_ref[1:2, :]
    before = (iota((TOKENS, TOKENS), 0) < iota((TOKENS, TOKENS), 1)).astype(F32).astype(BF16)

    def home_of(place):
        delta = jnp.zeros_like(place)
        for p, d in enumerate(DELTA):
            delta = jnp.where(place == p, d, delta)
        return lax.rem(z + delta, ZS)

    row = iota((ZS * 8, 1), 0)
    expert = jnp.where(row % 8 < XS, home_of(row // 8) * XS + row % 8, -1)
    first, second = ids0 == expert, ids1 == expert
    chosen = (first | second).astype(F32)
    rank1 = (nn_dot(chosen.astype(BF16), before) + 1.0) * chosen
    weight = jnp.where(first, rw0, 0.0) + jnp.where(second, rw1, 0.0)
    w_hi = weight.astype(BF16).astype(F32)
    w_lo = weight - w_hi
    place8 = iota((ZS, 1), 0)
    in_group = (ids0 // XS == home_of(place8)).astype(F32)
    slot = nn_dot(in_group.astype(BF16), before) + (place8 * SLOT).astype(F32)
    spot = jnp.sum(in_group * slot, axis=0, keepdims=True).astype(jnp.int32)
    for p in range(ZS):
        onehot[p] = (iota((SLOT, TOKENS), 0) + p * SLOT == spot).astype(F32).astype(BF16)

    pl.semaphore_wait(barrier, len(partners))

    low, high = pl.ds(0, HALF), pl.ds(HALF, HALF)

    def part(name, m, h):
        if name == "near":
            return near.at[:, m, (low, high)[h]]
        return (far.at[0, m], far.at[1, m, low], far.at[1, m, high], far.at[2, m])[h]

    def ring(name, h, step, send, recv):
        k = step - 1
        pairs = [
            (part(name, step - 1, h), part(name, step, h)),
            (part(name, (YS - step + 1) % YS, h), part(name, YS - step, h)),
        ]
        if step == 4 and name == "near":
            pairs[1 - h] = None
        elif step == 4 and h in (1, 2):
            pairs[2 - h] = None
        elif step == 4:
            w = (0, 1, 1, 2)[h]
            pairs = [(far.at[w, 3, low], far.at[w, 4, low]), (far.at[w, 5, high], far.at[w, 4, high])]
        return [
            remote(*pair, send.at[h, way, k], recv.at[h, way, k], at_y((1, YS - 1)[way]))
            for way, pair in enumerate(pairs) if pair is not None
        ]

    rings, dies = {}, {}
    for name, count, sems in (
        ("near", 2, (ws_sem, wr_sem, ds_sem, dr_sem)), ("far", 4, (fs_sem, fr_sem, gs_sem, gr_sem))
    ):
        for h in range(count):
            for step in (1, 2, 3, 4):
                rings[name, h, step] = ring(name, h, step, *sems[:2])
            for m in range(YS):
                dies[name, h, m] = remote(
                    part(name, m, h), part(name, YS + m, h), sems[2].at[h, m], sems[3].at[h, m], other
                )

    own = (near.at[0, 0], near.at[1, 0, low], near.at[1, 0, high], near.at[2, 0])
    shards = [
        remote(own[h], part("far", 0, h), hs_sem.at[h], hr_sem.at[h], at_z(4)) for h in range(4)
    ]

    def relay(name, step, *chains):
        for h in chains:
            if step > 0:
                for copy in rings[name, h, step]:
                    copy.wait_recv()
            elif name == "far":
                shards[h].wait_recv()
            if step < 4:
                for copy in rings[name, h, step + 1]:
                    copy.start()
        for h in chains:
            for m in sorted({step, (YS - step) % YS}):
                dies[name, h, m].start()

    def whole(name):
        for key, copy in dies.items():
            if key[0] == name:
                copy.wait_recv()

    z_out, m_out = {}, {}

    def send_plane(p):
        chosen_rows = onehot[p]
        meta = jnp.concatenate(
            [rank1[8 * p : 8 * p + 8], w_hi[8 * p : 8 * p + 8], w_lo[8 * p : 8 * p + 8],
             jnp.zeros((8, TOKENS), F32)], axis=0,
        ).astype(BF16)
        meta = nt_dot(meta, chosen_rows).astype(BF16)
        meta = jnp.concatenate([meta, jnp.zeros((32, 128 - SLOT), BF16)], axis=1)
        to_rows, to_meta = (zrecv, mrecv) if p in LOCAL else (zsend, msend)
        to_meta[p] = meta
        for c in range(0, WIDTH, COLS):
            block = nn_dot(chosen_rows, normed[:, c : c + COLS])
            to_rows[p, :, c : c + COLS] = block.astype(BF16)
        if p not in LOCAL:
            m_out[p] = remote(msend.at[p], mrecv.at[p], ms_sem.at[p], mr_sem.at[p], at_z(STEP[p]))
            z_out[p] = remote(zsend.at[p], zrecv.at[p], zs_sem.at[p], zr_sem.at[p], at_z(STEP[p]))
            m_out[p].start()
            z_out[p].start()

    def selector(p):
        meta = mrecv[p].astype(F32)[:, :SLOT]
        want = (iota((CAP, SLOT), 0) + 1).astype(F32)
        return meta, [(meta[i : i + 1, :] == want).astype(F32) for i in range(XS)]

    x_out, o_out = {}, {}

    def send_experts(p):
        if p not in LOCAL:
            m_out[p].wait_recv()
            z_out[p].wait_recv()
        pick = jnp.concatenate(selector(p)[1], axis=0).astype(BF16)
        for c in range(0, WIDTH, COLS):
            block = nn_dot(pick, zrecv[p, :, c : c + COLS]).astype(BF16)
            xsend[p, :, :, c : c + COLS] = block.reshape(XS, CAP, COLS)
        for j, step in enumerate(STEP_X):
            x_out[p, j] = remote(
                xsend.at[p, lax.rem(x + step, XS)], xrecv.at[p, j + 1],
                xs_sem.at[p, j], xr_sem.at[p, j], at_x(step),
            )
            x_out[p, j].start()
        xrecv[p, 0] = xsend[p, x]

    def experts(p, count, weights):
        for q in range(p, p + count):
            for j in range(XS - 1):
                x_out[q, j].wait_recv()
        rows = xrecv[pl.ds(p, count)].reshape(count * XS * CAP, WIDTH)
        gate = nt_dot(rows, weights[0].reshape(FF, WIDTH))
        up = nt_dot(rows, weights[1].reshape(FF, WIDTH))
        hidden = (gate / (1.0 + jnp.exp(-gate)) * up).astype(BF16)
        for c in range(0, WIDTH, COLS):
            block = nn_dot(hidden, weights[2, :, :, c : c + COLS].reshape(FF, COLS)).astype(BF16)
            ores[pl.ds(p, count), :, :, c : c + COLS] = block.reshape(count, XS, CAP, COLS)
        for q in range(p, p + count):
            for j, step in enumerate(STEP_X):
                o_out[q, j] = remote(
                    ores.at[q, j + 1], xret.at[q, x],
                    os_sem.at[q, j], or_sem.at[q, j], at_x(XS - step),
                )
                o_out[q, j].start()
            xret[q, x] = ores[q, 0]

    b_out = {}

    def combine(p):
        for j, step in enumerate(STEP_X):
            remote(
                ores.at[p, j + 1], xret.at[p, lax.rem(x + step, XS)],
                os_sem.at[p, j], or_sem.at[p, j], at_x(XS - step),
            ).wait_recv()
        meta, picks = selector(p)
        hi = jnp.concatenate(
            [pick * meta[8 + i : 9 + i, :] for i, pick in enumerate(picks)], axis=0
        ).astype(BF16)
        lo = jnp.concatenate(
            [pick * meta[16 + i : 17 + i, :] for i, pick in enumerate(picks)], axis=0
        ).astype(BF16)
        to_rows = zfin if p in LOCAL else zback
        for c in range(0, WIDTH, COLS):
            rows = xret[p, :, :, c : c + COLS].reshape(XS * CAP, COLS)
            to_rows[p, :, c : c + COLS] = (tn_dot(hi, rows) + tn_dot(lo, rows)).astype(BF16)
        if p not in LOCAL:
            b_out[p] = remote(
                zback.at[p], zfin.at[p], bs_sem.at[p], br_sem.at[p], at_z(ZS - STEP[p])
            )
            b_out[p].start()

    def unsort(first, count, more):
        for p in range(first, first + count):
            if p not in LOCAL:
                b_out[p].wait_recv()
        picks = onehot[pl.ds(first, count)].reshape(count * SLOT, TOKENS)
        for c in range(0, WIDTH, COLS):
            rows = zfin[pl.ds(first, count), :, c : c + COLS].reshape(count * SLOT, COLS)
            block = tn_dot(picks, rows)
            mixed[:, c : c + COLS] = mixed[:, c : c + COLS] + block if more else block

    relay("near", 0, 0, 1)
    send_plane(6)
    send_experts(6)
    send_plane(0)
    send_plane(1)
    send_plane(7)
    send_experts(7)
    send_plane(4)
    send_plane(5)
    shards[0].start()
    shards[1].start()
    send_plane(2)
    send_plane(3)
    relay("near", 1, 0)
    send_experts(0)
    send_experts(1)
    relay("near", 1, 1)
    relay("near", 2, 0)
    relay("near", 2, 1)
    send_experts(4)
    send_experts(5)
    relay("near", 3, 0)
    relay("near", 3, 1)
    relay("far", 0, 0, 1)
    relay("near", 4, 0)
    relay("near", 4, 1)
    send_experts(2)
    send_experts(3)
    shards[2].start()
    shards[3].start()
    relay("far", 1, 0, 1)
    relay("far", 2, 0, 1)
    whole("near")
    experts(0, 2, near)
    relay("far", 0, 2, 3)
    relay("far", 3, 0, 1)
    experts(2, 2, near)
    relay("far", 1, 2, 3)
    relay("far", 4, 0, 1)
    experts(6, 1, near)
    relay("far", 2, 2, 3)
    combine(0)
    combine(1)
    relay("far", 3, 2, 3)
    combine(2)
    relay("far", 4, 2, 3)
    whole("far")
    experts(4, 2, far)
    combine(3)
    experts(7, 1, far)
    combine(6)
    combine(4)
    combine(5)
    unsort(0, 4, False)
    combine(7)
    unsort(4, 4, True)
    for r in range(0, TOKENS, 32):
        out_ref[pl.ds(r, 32), :] = rms_scale(mixed[pl.ds(r, 32), :], post_ref[...]).astype(BF16)
    for copies in [*rings.values(), dies.values(), shards]:
        for copy in copies:
            copy.wait_send()
    for copies in (m_out, z_out, x_out, o_out, b_out):
        for copy in copies.values():
            copy.wait_send()


def body(tokens, pre_gain, post_gain, expert_ids, route_weight, w_gate, w_up, w_down):
    dma = pltpu.SemaphoreType.DMA
    vmem = pltpu.VMEM
    return pl.pallas_call(
        kernel,
        name="experts",
        out_shape=jax.ShapeDtypeStruct((TOKENS, WIDTH), BF16),
        in_specs=[pl.BlockSpec(memory_space=pltpu.HBM)] * 8,
        out_specs=pl.BlockSpec(memory_space=vmem),
        scratch_shapes=[
            vmem((TOKENS, WIDTH), BF16),
            vmem((1, WIDTH), F32),
            vmem((1, WIDTH), F32),
            vmem((2, TOKENS), jnp.int32),
            vmem((2, TOKENS), F32),
            dma((8,)),
            vmem((TOKENS, WIDTH), BF16),
            vmem((ZS, SLOT, TOKENS), BF16),
            vmem((ZS, SLOT, WIDTH), BF16),
            vmem((ZS, 32, 128), BF16),
            vmem((ZS, SLOT, WIDTH), BF16),
            vmem((ZS, 32, 128), BF16),
            vmem((ZS, XS, CAP, WIDTH), BF16),
            vmem((ZS, XS, CAP, WIDTH), BF16),
            vmem((3, 2 * YS, PART, WIDTH), BF16),
            vmem((3, 2 * YS, PART, WIDTH), BF16),
            vmem((ZS, XS, CAP, WIDTH), BF16),
            vmem((ZS, XS, CAP, WIDTH), BF16),
            vmem((ZS, SLOT, WIDTH), BF16),
            vmem((ZS, SLOT, WIDTH), BF16),
            vmem((TOKENS, WIDTH), F32),
            dma((ZS,)), dma((ZS,)), dma((ZS,)), dma((ZS,)),
            dma((ZS, XS - 1)), dma((ZS, XS - 1)), dma((ZS, XS - 1)), dma((ZS, XS - 1)),
            dma((ZS,)), dma((ZS,)),
            dma((2, 2, 4)), dma((2, 2, 4)), dma((2, YS)), dma((2, YS)),
            dma((4, 2, 4)), dma((4, 2, 4)), dma((4, YS)), dma((4, YS)), dma((4,)), dma((4,)),
        ],
        compiler_params=pltpu.CompilerParams(
            collective_id=0, has_side_effects=True, vmem_limit_bytes=52 << 20
        ),
    )(*[
        pltpu.with_memory_space_constraint(a, pltpu.HBM)
        for a in (
            tokens, pre_gain[None], post_gain[None], expert_ids.T, route_weight.T,
            w_gate[0].T, w_up[0].T, w_down[0].T,
        )
    ])


def solution(mesh):
    in_specs = (
        P(("ep", "tp"), None),
        P(),
        P(),
        P(("ep", "tp"), None),
        P(("ep", "tp"), None),
        P("ep", None, "tp"),
        P("ep", None, "tp"),
        P("ep", None, "tp"),
    )
    out_specs = P(("ep", "tp"), None)
    return jax.shard_map(body, mesh=mesh, in_specs=in_specs, out_specs=out_specs, check_vma=False)
```

```python
import jax
import jax.numpy as jnp
from jax import lax
from jax.experimental import pallas as pl
from jax.experimental.pallas import tpu as pltpu
from jax.sharding import PartitionSpec as P

MESH = pl.DeviceIdType.MESH
BF16 = jnp.bfloat16
F32 = jnp.float32
WIDTH = 2048
TOKENS = 256
PART = 32
FF = 512
ZS = 8
XS = 4
YS = 8
SLOT = 64
CAP = 32
COLS = 512
DELTA = (1, 7, 2, 6, 3, 5, 0, 4)
STEP = (1, 7, 2, 6, 7, 1, 0, 0)
LOCAL = (6, 7)
STEP_X = (1, 3, 2)
HALF = PART // 2
BLOCK = 64


def nt_dot(a, b):
    return lax.dot_general(a, b, (((1,), (1,)), ((), ())), preferred_element_type=F32)


def tn_dot(a, b):
    return lax.dot_general(a, b, (((0,), (0,)), ((), ())), preferred_element_type=F32)


def nn_dot(a, b):
    return jnp.dot(a, b, preferred_element_type=F32)


def iota(shape, dim):
    return lax.broadcasted_iota(jnp.int32, shape, dim)


def rms_scale(values, gain):
    mean_sq = jnp.mean(values * values, axis=-1, keepdims=True)
    return values * lax.rsqrt(mean_sq + 1e-06) * gain


def kernel(
    tok_hbm, pre_hbm, post_hbm, ids_hbm, rw_hbm, wg_hbm, wu_hbm, wd_hbm, out_ref,
    tok_ref, pre_ref, post_ref, ids_ref, rw_ref, in_sem, normed, onehot, zsend, msend, zrecv, mrecv, xsend, xrecv, near, far, ores, xret, zback, zfin, mixed, hid,
    zs_sem, zr_sem, ms_sem, mr_sem, xs_sem, xr_sem, os_sem, or_sem, bs_sem, br_sem,
    ws_sem, wr_sem, ds_sem, dr_sem, fs_sem, fr_sem, gs_sem, gr_sem, hs_sem, hr_sem,
):
    ep, tp = lax.axis_index("ep"), lax.axis_index("tp")
    z, x = ep // XS, ep % XS
    y, core = tp // 2, tp % 2

    def at_z(step):
        return (lax.rem(z + step, ZS) * XS + x, tp)

    def at_x(step):
        return (z * XS + lax.rem(x + step, XS), tp)

    def at_y(step):
        return (ep, lax.rem(y + step, YS) * 2 + core)

    other = (ep, y * 2 + (1 - core))

    def remote(src, dst, send, recv, device):
        return pltpu.make_async_remote_copy(
            src_ref=src, dst_ref=dst, send_sem=send, recv_sem=recv,
            device_id=device, device_id_type=MESH,
        )

    blocks = [pl.ds(r, BLOCK) for r in range(0, TOKENS, BLOCK)]
    loads = [
        pltpu.make_async_copy(src, dst, in_sem.at[k])
        for k, (src, dst) in enumerate((
            (ids_hbm, ids_ref), (rw_hbm, rw_ref), (pre_hbm, pre_ref),
            *[(tok_hbm.at[b], tok_ref.at[b]) for b in blocks],
            (wg_hbm, near.at[0, 0]), (wu_hbm, near.at[1, 0]), (wd_hbm, near.at[2, 0]),
            (post_hbm, post_ref),
        ))
    ]
    for copy in loads:
        copy.start()
    barrier = pltpu.get_barrier_semaphore()
    partners = [at_z(k) for k in (1, 2, 4, 6, 7)] + [at_x(k) for k in range(1, XS)]
    partners += [at_y(1), at_y(YS - 1), other]
    for device in partners:
        pl.semaphore_signal(barrier, inc=1, device_id=device, device_id_type=MESH)

    for copy in loads[:3]:
        copy.wait()
    ids0, ids1 = ids_ref[0:1, :], ids_ref[1:2, :]
    rw0, rw1 = rw_ref[0:1, :], rw_ref[1:2, :]
    before = (iota((TOKENS, TOKENS), 0) < iota((TOKENS, TOKENS), 1)).astype(F32).astype(BF16)

    def home_of(place):
        delta = jnp.zeros_like(place)
        for p, d in enumerate(DELTA):
            delta = jnp.where(place == p, d, delta)
        return lax.rem(z + delta, ZS)

    row = iota((ZS * 8, 1), 0)
    expert = jnp.where(row % 8 < XS, home_of(row // 8) * XS + row % 8, -1)
    first, second = ids0 == expert, ids1 == expert
    chosen = (first | second).astype(F32)
    rank1 = (nn_dot(chosen.astype(BF16), before) + 1.0) * chosen
    weight = jnp.where(first, rw0, 0.0) + jnp.where(second, rw1, 0.0)
    w_hi = weight.astype(BF16).astype(F32)
    w_lo = weight - w_hi
    place8 = iota((ZS, 1), 0)
    in_group = (ids0 // XS == home_of(place8)).astype(F32)
    slot = nn_dot(in_group.astype(BF16), before) + (place8 * SLOT).astype(F32)
    spot = jnp.sum(in_group * slot, axis=0, keepdims=True).astype(jnp.int32)
    for p in range(ZS):
        onehot[p] = (iota((SLOT, TOKENS), 0) + p * SLOT == spot).astype(F32).astype(BF16)

    for k, block in enumerate(blocks):
        loads[3 + k].wait()
        for r in range(0, BLOCK, 32):
            rows = pl.ds(k * BLOCK + r, 32)
            normed[rows, :] = rms_scale(tok_ref[rows, :].astype(F32), pre_ref[...]).astype(BF16)
    for copy in loads[3 + len(blocks) :]:
        copy.wait()

    pl.semaphore_wait(barrier, len(partners))

    low, high = pl.ds(0, HALF), pl.ds(HALF, HALF)

    def part(name, m, h):
        if name == "near":
            return near.at[:, m, (low, high)[h]]
        return (far.at[0, m], far.at[1, m, low], far.at[1, m, high], far.at[2, m])[h]

    def ring(name, h, step, send, recv):
        k = step - 1
        pairs = [
            (part(name, step - 1, h), part(name, step, h)),
            (part(name, (YS - step + 1) % YS, h), part(name, YS - step, h)),
        ]
        if step == 4 and name == "near":
            pairs[1 - h] = None
        elif step == 4 and h in (1, 2):
            pairs[2 - h] = None
        elif step == 4:
            w = (0, 1, 1, 2)[h]
            pairs = [(far.at[w, 3, low], far.at[w, 4, low]), (far.at[w, 5, high], far.at[w, 4, high])]
        return [
            remote(*pair, send.at[h, way, k], recv.at[h, way, k], at_y((1, YS - 1)[way]))
            for way, pair in enumerate(pairs) if pair is not None
        ]

    rings, dies = {}, {}
    for name, count, sems in (
        ("near", 2, (ws_sem, wr_sem, ds_sem, dr_sem)), ("far", 4, (fs_sem, fr_sem, gs_sem, gr_sem))
    ):
        for h in range(count):
            for step in (1, 2, 3, 4):
                rings[name, h, step] = ring(name, h, step, *sems[:2])
            for m in range(YS):
                dies[name, h, m] = remote(
                    part(name, m, h), part(name, YS + m, h), sems[2].at[h, m], sems[3].at[h, m], other
                )

    own = (near.at[0, 0], near.at[1, 0, low], near.at[1, 0, high], near.at[2, 0])
    shards = [
        remote(own[h], part("far", 0, h), hs_sem.at[h], hr_sem.at[h], at_z(4)) for h in range(4)
    ]

    def relay(name, step, *chains):
        for h in chains:
            if step > 0:
                for copy in rings[name, h, step]:
                    copy.wait_recv()
            elif name == "far":
                shards[h].wait_recv()
            if step < 4:
                for copy in rings[name, h, step + 1]:
                    copy.start()
        for h in chains:
            for m in sorted({step, (YS - step) % YS}):
                dies[name, h, m].start()

    def whole(name):
        for key, copy in dies.items():
            if key[0] == name:
                copy.wait_recv()

    z_out, m_out = {}, {}

    def send_plane(p):
        chosen_rows = onehot[p]
        meta = jnp.concatenate(
            [rank1[8 * p : 8 * p + 8], w_hi[8 * p : 8 * p + 8], w_lo[8 * p : 8 * p + 8],
             jnp.zeros((8, TOKENS), F32)], axis=0,
        ).astype(BF16)
        meta = nt_dot(meta, chosen_rows).astype(BF16)
        meta = jnp.concatenate([meta, jnp.zeros((32, 128 - SLOT), BF16)], axis=1)
        to_rows, to_meta = (zrecv, mrecv) if p in LOCAL else (zsend, msend)
        to_meta[p] = meta
        for c in range(0, WIDTH, COLS):
            block = nn_dot(chosen_rows, normed[:, c : c + COLS])
            to_rows[p, :, c : c + COLS] = block.astype(BF16)
        if p not in LOCAL:
            m_out[p] = remote(msend.at[p], mrecv.at[p], ms_sem.at[p], mr_sem.at[p], at_z(STEP[p]))
            z_out[p] = remote(zsend.at[p], zrecv.at[p], zs_sem.at[p], zr_sem.at[p], at_z(STEP[p]))
            m_out[p].start()
            z_out[p].start()

    def selector(p):
        meta = mrecv[p].astype(F32)[:, :SLOT]
        want = (iota((CAP, SLOT), 0) + 1).astype(F32)
        return meta, [(meta[i : i + 1, :] == want).astype(F32) for i in range(XS)]

    x_out, o_out = {}, {}

    def send_experts(p):
        if p not in LOCAL:
            m_out[p].wait_recv()
            z_out[p].wait_recv()
        pick = jnp.concatenate(selector(p)[1], axis=0).astype(BF16)
        for c in range(0, WIDTH, COLS):
            block = nn_dot(pick, zrecv[p, :, c : c + COLS]).astype(BF16)
            xsend[p, :, :, c : c + COLS] = block.reshape(XS, CAP, COLS)
        for j, step in enumerate(STEP_X):
            x_out[p, j] = remote(
                xsend.at[p, lax.rem(x + step, XS)], xrecv.at[p, j + 1],
                xs_sem.at[p, j], xr_sem.at[p, j], at_x(step),
            )
            x_out[p, j].start()
        xrecv[p, 0] = xsend[p, x]

    def units(p, count, weights, half):
        if half == 0:
            for q in range(p, p + count):
                for j in range(XS - 1):
                    x_out[q, j].wait_recv()
        rows = xrecv[pl.ds(p, count)].reshape(count * XS * CAP, WIDTH)
        own_half = pl.ds(half * YS, YS)
        gate = nt_dot(rows, weights[0, own_half].reshape(FF // 2, WIDTH))
        up = nt_dot(rows, weights[1, own_half].reshape(FF // 2, WIDTH))
        part_hidden = (gate / (1.0 + jnp.exp(-gate)) * up).astype(BF16)
        at = half * (FF // 2)
        hid[pl.ds(p, count), :, at : at + FF // 2] = part_hidden.reshape(count, XS * CAP, FF // 2)

    def experts(p, count, weights, started=False):
        if not started:
            units(p, count, weights, 0)
        units(p, count, weights, 1)
        hidden = hid[pl.ds(p, count)].reshape(count * XS * CAP, FF)
        for c in range(0, WIDTH, COLS):
            block = nn_dot(hidden, weights[2, :, :, c : c + COLS].reshape(FF, COLS)).astype(BF16)
            ores[pl.ds(p, count), :, :, c : c + COLS] = block.reshape(count, XS, CAP, COLS)
        for q in range(p, p + count):
            for j, step in enumerate(STEP_X):
                o_out[q, j] = remote(
                    ores.at[q, j + 1], xret.at[q, x],
                    os_sem.at[q, j], or_sem.at[q, j], at_x(XS - step),
                )
                o_out[q, j].start()
            xret[q, x] = ores[q, 0]

    b_out = {}

    def combine(p):
        for j, step in enumerate(STEP_X):
            remote(
                ores.at[p, j + 1], xret.at[p, lax.rem(x + step, XS)],
                os_sem.at[p, j], or_sem.at[p, j], at_x(XS - step),
            ).wait_recv()
        meta, picks = selector(p)
        hi = jnp.concatenate(
            [pick * meta[8 + i : 9 + i, :] for i, pick in enumerate(picks)], axis=0
        ).astype(BF16)
        lo = jnp.concatenate(
            [pick * meta[16 + i : 17 + i, :] for i, pick in enumerate(picks)], axis=0
        ).astype(BF16)
        to_rows = zfin if p in LOCAL else zback
        for c in range(0, WIDTH, COLS):
            rows = xret[p, :, :, c : c + COLS].reshape(XS * CAP, COLS)
            to_rows[p, :, c : c + COLS] = (tn_dot(hi, rows) + tn_dot(lo, rows)).astype(BF16)
        if p not in LOCAL:
            b_out[p] = remote(
                zback.at[p], zfin.at[p], bs_sem.at[p], br_sem.at[p], at_z(ZS - STEP[p])
            )
            b_out[p].start()

    def unsort(first, count, more):
        for p in range(first, first + count):
            if p not in LOCAL:
                b_out[p].wait_recv()
        picks = onehot[pl.ds(first, count)].reshape(count * SLOT, TOKENS)
        for c in range(0, WIDTH, COLS):
            rows = zfin[pl.ds(first, count), :, c : c + COLS].reshape(count * SLOT, COLS)
            block = tn_dot(picks, rows)
            mixed[:, c : c + COLS] = mixed[:, c : c + COLS] + block if more else block

    relay("near", 0, 0, 1)
    send_plane(6)
    send_experts(6)
    send_plane(0)
    send_plane(1)
    send_plane(7)
    send_experts(7)
    send_plane(4)
    send_plane(5)
    shards[0].start()
    shards[1].start()
    send_plane(2)
    send_plane(3)
    relay("near", 1, 0)
    send_experts(0)
    send_experts(1)
    relay("near", 1, 1)
    relay("near", 2, 0)
    relay("near", 2, 1)
    send_experts(4)
    send_experts(5)
    relay("near", 3, 0)
    relay("near", 3, 1)
    relay("far", 0, 0, 1)
    relay("near", 4, 0)
    relay("near", 4, 1)
    send_experts(2)
    send_experts(3)
    shards[2].start()
    shards[3].start()
    relay("far", 1, 0, 1)
    relay("far", 2, 0, 1)
    whole("near")
    experts(0, 2, near)
    relay("far", 0, 2, 3)
    relay("far", 3, 0, 1)
    experts(2, 2, near)
    relay("far", 1, 2, 3)
    relay("far", 4, 0, 1)
    experts(6, 1, near)
    relay("far", 2, 2, 3)
    combine(0)
    combine(1)
    relay("far", 3, 2, 3)
    combine(2)
    relay("far", 4, 2, 3)
    units(4, 2, far, 0)
    whole("far")
    experts(4, 2, far, True)
    combine(3)
    experts(7, 1, far)
    combine(6)
    combine(4)
    combine(5)
    unsort(0, 4, False)
    combine(7)
    unsort(4, 4, True)
    for r in range(0, TOKENS, 32):
        out_ref[pl.ds(r, 32), :] = rms_scale(mixed[pl.ds(r, 32), :], post_ref[...]).astype(BF16)
    for copies in [*rings.values(), dies.values(), shards]:
        for copy in copies:
            copy.wait_send()
    for copies in (m_out, z_out, x_out, o_out, b_out):
        for copy in copies.values():
            copy.wait_send()


def body(tokens, pre_gain, post_gain, expert_ids, route_weight, w_gate, w_up, w_down):
    dma = pltpu.SemaphoreType.DMA
    vmem = pltpu.VMEM
    return pl.pallas_call(
        kernel,
        name="experts",
        out_shape=jax.ShapeDtypeStruct((TOKENS, WIDTH), BF16),
        in_specs=[pl.BlockSpec(memory_space=pltpu.HBM)] * 8,
        out_specs=pl.BlockSpec(memory_space=vmem),
        scratch_shapes=[
            vmem((TOKENS, WIDTH), BF16),
            vmem((1, WIDTH), F32),
            vmem((1, WIDTH), F32),
            vmem((2, TOKENS), jnp.int32),
            vmem((2, TOKENS), F32),
            dma((7 + TOKENS // BLOCK,)),
            vmem((TOKENS, WIDTH), BF16),
            vmem((ZS, SLOT, TOKENS), BF16),
            vmem((ZS, SLOT, WIDTH), BF16),
            vmem((ZS, 32, 128), BF16),
            vmem((ZS, SLOT, WIDTH), BF16),
            vmem((ZS, 32, 128), BF16),
            vmem((ZS, XS, CAP, WIDTH), BF16),
            vmem((ZS, XS, CAP, WIDTH), BF16),
            vmem((3, 2 * YS, PART, WIDTH), BF16),
            vmem((3, 2 * YS, PART, WIDTH), BF16),
            vmem((ZS, XS, CAP, WIDTH), BF16),
            vmem((ZS, XS, CAP, WIDTH), BF16),
            vmem((ZS, SLOT, WIDTH), BF16),
            vmem((ZS, SLOT, WIDTH), BF16),
            vmem((TOKENS, WIDTH), F32),
            vmem((ZS, XS * CAP, FF), BF16),
            dma((ZS,)), dma((ZS,)), dma((ZS,)), dma((ZS,)),
            dma((ZS, XS - 1)), dma((ZS, XS - 1)), dma((ZS, XS - 1)), dma((ZS, XS - 1)),
            dma((ZS,)), dma((ZS,)),
            dma((2, 2, 4)), dma((2, 2, 4)), dma((2, YS)), dma((2, YS)),
            dma((4, 2, 4)), dma((4, 2, 4)), dma((4, YS)), dma((4, YS)), dma((4,)), dma((4,)),
        ],
        compiler_params=pltpu.CompilerParams(
            collective_id=0, has_side_effects=True, vmem_limit_bytes=52 << 20
        ),
    )(*[
        pltpu.with_memory_space_constraint(a, pltpu.HBM)
        for a in (
            tokens, pre_gain[None], post_gain[None], expert_ids.T, route_weight.T,
            w_gate[0].T, w_up[0].T, w_down[0].T,
        )
    ])


def solution(mesh):
    in_specs = (
        P(("ep", "tp"), None),
        P(),
        P(),
        P(("ep", "tp"), None),
        P(("ep", "tp"), None),
        P("ep", None, "tp"),
        P("ep", None, "tp"),
        P("ep", None, "tp"),
    )
    out_specs = P(("ep", "tp"), None)
    return jax.shard_map(body, mesh=mesh, in_specs=in_specs, out_specs=out_specs, check_vma=False)
```
